32 devices in a mesh: ep: 8 (over z, y), tp: 4 (over x, core).
Axes of the slice: x: 2, y: 2, z: 4, core: 2. Of those that a mesh axis runs over, the one named last changes fastest.
Arguments:
- value_in: bfloat16 [4096, 2048], P('ep', 'tp'), may hold values from -400 to 400
- gate_in: bfloat16 [4096, 2048], P('ep', 'tp'), may hold values from -8 to 8
- conv_taps: float32 [31, 2048], P(None, 'tp'), may hold values from -1 to 1
- conv_bias: float32 [2048], P('tp'), may hold values from -3 to 3
- ln_gain: float32 [2048], P('tp'), may hold values from 0.1 to 1.9
- ln_bias: float32 [2048], P('tp'), may hold values from -3 to 3
- out_proj: bfloat16 [2048, 4096], P('tp'), may hold values from -0.125 to 0.125
- tokens_b: bfloat16 [4096, 4096], P('ep'), may hold values from -6 to 6
- norm_gain: float32 [4096], replicated, may hold values from 0.1 to 1.9
- routes: int32 [4096, 2], P(('ep', 'tp')), may hold values from 0 to 7, all different within a row; in each aligned block of 128 rows (0 to 127, 128 to 255, ...) at most 48 rows name the same one
- route_weights: float32 [4096, 2], P(('ep', 'tp')), may hold values from 0.2 to 1.5
- expert_gate: bfloat16 [8, 4096, 1024], P('ep', None, 'tp'), may hold values from -0.09375 to 0.09375
- expert_up: bfloat16 [8, 4096, 1024], P('ep', None, 'tp'), may hold values from -0.09375 to 0.09375
- expert_down: bfloat16 [8, 1024, 4096], P('ep', 'tp'), may hold values from -0.1875 to 0.1875
- shared_gate: bfloat16 [4096, 1024], P(None, 'tp'), may hold values from -0.09375 to 0.09375
- shared_up: bfloat16 [4096, 1024], P(None, 'tp'), may hold values from -0.09375 to 0.09375
- shared_down: bfloat16 [1024, 4096], P('tp'), may hold values from -0.1875 to 0.1875
Outputs:
- mixer_out: bfloat16 [4096, 4096], P(('ep', 'tp'))
- experts_out: bfloat16 [4096, 4096], P(('ep', 'tp'))
The draws below stay inside these ranges and needn't reach their ends.
Inputs may be any that keep to these rules, and one draw needn't show every extreme that they name: `routes`: each row names 2 different experts. In each aligned block of 128 rows (the rows of one device) no expert is named by more than 48 rows, and in some blocks an expert is named by exactly 48 rows.
All inputs are finite; a program needn't handle non-finite values.
Results may differ from the reference program's by a relative error of at most 0.012.
Values may be sent and summed in bfloat16 or wider, within the bound.
A program may use at most 128 MiB of HBM per device.

```python
import math
from functools import partial
import jax
import jax.numpy as jnp
import numpy as np
from jax import lax

D = 4096
CHANNELS = 2048
EXPERT_WIDTH = 1024
TAPS = 31
TOP_K = 2
ROWS_DEV = 128
EXPERTS = 8
CAP = 48
SEQ_LEN = 4096
TOKENS_B = 4096
N_TP = 4


def draw_value_in(key, part):
    keys = jax.random.split(jax.random.fold_in(key, 11), 2)
    base = jnp.clip(jax.random.normal(keys[0], (SEQ_LEN, CHANNELS), jnp.float32), -5.0, 5.0)
    column = jnp.arange(CHANNELS, dtype=jnp.float32) / CHANNELS
    rough = jax.random.uniform(keys[1], (CHANNELS,), jnp.float32, 0.5, 1.5)
    scales = 0.3 * 10.0 ** column * rough
    values = base * scales[None, :]
    return values.astype(jnp.bfloat16)


def levels(key, dims, shards, least, largest):
    gain, own = 1.0, jax.random.fold_in(key, 6)
    for position, shards_of in shards:
        draws = jnp.exp(jax.random.uniform(jax.random.fold_in(own, position), (shards_of,), jnp.float32, least / len(shards), largest / len(shards)))
        gain = gain * jnp.repeat(draws, dims[position] // shards_of).reshape([-1 if axis == position else 1 for axis in range(len(dims))])
    return gain


def deal_out(rng, own, number, rows, amount, top, limit, lean):
    order = jax.random.permutation(rng, amount)
    heavy_load, ordinary = load_shares(amount, rows * top, limit, lean, True), load_shares(amount, rows * top, limit, lean, False)
    places = jnp.arange(amount)

    def named(sizes, offset_by):
        used = int((sizes > 0).sum())
        fixed = max(1, used // 4)
        shifted = fixed + (places - fixed + offset_by * (used - fixed)) % max(1, amount - fixed)
        return jnp.zeros((amount,), jnp.int32).at[order[jnp.where(places < fixed, places, shifted)]].set(jnp.asarray(sizes, jnp.int32))

    sizes = jnp.where(number % 4 == 0, named(heavy_load, number // 4), named(ordinary, number - number // 4 - 1))
    mixed = jax.random.permutation(jax.random.fold_in(own, 3), amount)
    giver, sink = mixed[0:amount // 2 * 2:2], mixed[1:amount // 2 * 2:2]
    slack = jnp.minimum(sizes[giver] - 1, limit - sizes[sink]) // 2
    slack = jnp.where((giver == order[0]) | (sink == order[0]) | (sizes[sink] == 0), 0, jnp.maximum(slack, 0))
    shifted = jax.random.randint(jax.random.fold_in(own, 4), (amount // 2,), 0, 1 << 20) % (slack + 1)
    sizes = sizes.at[giver].add(-shifted).at[sink].add(shifted)
    labels = jnp.searchsorted(jnp.cumsum(sizes), jnp.arange(rows * top), side="right").astype(jnp.int32)
    table = labels.reshape(top, rows).T
    table = table[jax.random.permutation(jax.random.fold_in(own, 1), rows)]
    offset_by = jax.random.randint(jax.random.fold_in(own, 2), (rows, 1), 0, top)
    return jnp.take_along_axis(table, (jnp.arange(top)[None, :] + offset_by) % top, axis=1)


def load_shares(number_of, total, most, lean, full):
    portions = [(1 << 20) // math.isqrt(rank ** lean) + 1 for rank in range(1, number_of + 1)]
    largest = most if full else min(most, max(-(-total // number_of), total * portions[0] // sum(portions)))
    least = 1 if total - largest >= number_of - 1 else 0
    holding, rest = [largest] + [least] * (number_of - 1), total - largest - least * (number_of - 1)
    while rest > 0:
        free = [i for i in range(1, number_of) if holding[i] < largest] or [i for i in range(1, number_of) if holding[i] < most]
        whole, left = sum([portions[i] for i in free]), rest
        for i in free:
            addition = min(most - holding[i], max(1, left * portions[i] // whole), rest)
            holding[i] = holding[i] + addition
            rest = rest - addition
    return np.array(holding)


def normal_values(key, dims, deviation, bound, pieces=(), kind=jnp.bfloat16):
    values = jax.random.normal(key, dims, jnp.float32) * deviation
    if len(pieces) > 0:
        values = levels(key, dims, pieces, -0.22, 0.18) * values
    return jnp.clip(values, min=-bound, max=bound).astype(kind)


def setup_inputs(seed: int = 0) -> dict:
    key_of = jax.random.split(jax.random.key(seed), 18)
    value_in = draw_value_in(jax.random.fold_in(key_of[17], 71), 0)
    gate_in = normal_values(key_of[1], (SEQ_LEN, CHANNELS), 1.5, 8.0, ((0, 8), (1, 4)))
    conv_taps = normal_values(key_of[2], (TAPS, CHANNELS), TAPS ** -0.5, 1.0, ((1, 4),), jnp.float32)
    conv_bias = normal_values(key_of[3], (CHANNELS,), 0.5, 3.0, ((0, 4),), jnp.float32)
    ln_gain = jnp.clip(1.0 + 0.18 * jax.random.normal(key_of[4], (CHANNELS,), jnp.float32), 0.1, 1.9)
    ln_bias = normal_values(key_of[5], (CHANNELS,), 0.5, 3.0, ((0, 4),), jnp.float32)
    out_proj = normal_values(key_of[6], (CHANNELS, D), CHANNELS ** -0.5, 0.125, ((0, 4),))
    tokens_b = normal_values(key_of[7], (TOKENS_B, D), 1.0, 6.0, ((0, 8),))
    norm_gain = jnp.clip(1.0 + 0.18 * jax.random.normal(key_of[8], (D,), jnp.float32), 0.1, 1.9)
    routes_keys = jax.random.split(jax.random.fold_in(key_of[9], 1), TOKENS_B // ROWS_DEV)
    routes_turns = jax.random.permutation(jax.random.fold_in(key_of[9], 3), TOKENS_B // ROWS_DEV)
    routes = jax.vmap(lambda own, number: deal_out(jax.random.fold_in(key_of[9], 2), own, number, ROWS_DEV, EXPERTS, TOP_K, CAP, 1))(routes_keys, routes_turns).reshape((TOKENS_B, TOP_K))
    route_weights = jnp.clip(0.2 + 1.3 * jax.random.uniform(key_of[10], (TOKENS_B, TOP_K), jnp.float32) ** levels(key_of[10], (TOKENS_B, TOP_K), ((0, 32),), -0.2, 0.2), 0.2, 1.5)
    expert_gate = normal_values(key_of[11], (EXPERTS, D, EXPERT_WIDTH), D ** -0.5, 0.09375, ((0, 8), (2, 4)))
    expert_up = normal_values(key_of[12], (EXPERTS, D, EXPERT_WIDTH), D ** -0.5, 0.09375, ((0, 8), (2, 4)))
    expert_down = normal_values(key_of[13], (EXPERTS, EXPERT_WIDTH, D), EXPERT_WIDTH ** -0.5, 0.1875, ((0, 8), (1, 4)))
    shared_gate = normal_values(key_of[14], (D, EXPERT_WIDTH), D ** -0.5, 0.09375, ((1, 4),))
    shared_up = normal_values(key_of[15], (D, EXPERT_WIDTH), D ** -0.5, 0.09375, ((1, 4),))
    shared_down = normal_values(key_of[16], (EXPERT_WIDTH, D), EXPERT_WIDTH ** -0.5, 0.1875, ((0, 4),))
    return dict(value_in=value_in, gate_in=gate_in, conv_taps=conv_taps, conv_bias=conv_bias, ln_gain=ln_gain, ln_bias=ln_bias, out_proj=out_proj, tokens_b=tokens_b, norm_gain=norm_gain, routes=routes, route_weights=route_weights, expert_gate=expert_gate, expert_up=expert_up, expert_down=expert_down, shared_gate=shared_gate, shared_up=shared_up, shared_down=shared_down)


EPSILON = 1e-06

def round_trip(values):
    return lax.optimization_barrier(values.astype(jnp.bfloat16)).astype(jnp.float32)

def blocked_product(hidden, weight):
    block_rows = hidden.shape[1] // N_TP
    summed = jnp.zeros((hidden.shape[0], weight.shape[1]), jnp.float32)
    for block in range(N_TP):
        partial_sum = jnp.dot(hidden[:, block * block_rows:(block + 1) * block_rows], weight[block * block_rows:(block + 1) * block_rows], preferred_element_type=jnp.float32)
        summed = summed + round_trip(partial_sum)
    return summed.astype(jnp.bfloat16)

def gated_ffn(rows_in, weight_gate, weight_up, weight_down):
    hidden = (jax.nn.silu(jnp.dot(rows_in, weight_gate, preferred_element_type=jnp.float32)) * jnp.dot(rows_in, weight_up, preferred_element_type=jnp.float32)).astype(jnp.bfloat16)
    return blocked_product(hidden, weight_down)

def slot_table(route_ids, expert_count):
    chosen = route_ids.reshape(-1)
    onehot = (chosen[:, None] == jnp.arange(expert_count, dtype=jnp.int32)[None, :]).astype(jnp.int32)
    earlier = jnp.cumsum(onehot, axis=0) - onehot
    return (chosen, lax.optimization_barrier(jnp.sum(earlier * onehot, axis=1)).astype(jnp.int32))

def reference(value_in, gate_in, conv_taps, conv_bias, ln_gain, ln_bias, out_proj, tokens_b, norm_gain, routes, route_weights, expert_gate, expert_up, expert_down, shared_gate, shared_up, shared_down):
    gated = round_trip(value_in.astype(jnp.float32) * jax.nn.sigmoid(gate_in.astype(jnp.float32)))
    padded = jnp.concatenate([jnp.zeros((TAPS - 1, CHANNELS), jnp.float32), gated], axis=0)
    filtered = jnp.zeros((SEQ_LEN, CHANNELS), jnp.float32) + conv_bias[None, :]
    for tap_index in range(TAPS):
        filtered = filtered + conv_taps[tap_index][None, :] * padded[tap_index:tap_index + SEQ_LEN]
    average = lax.optimization_barrier(jnp.sum(filtered, axis=1)) / CHANNELS
    variance = lax.optimization_barrier(jnp.sum(filtered * filtered, axis=1)) / CHANNELS - average * average
    normed_a = (filtered - average[:, None]) * lax.rsqrt(variance[:, None] + EPSILON) * ln_gain + ln_bias
    activated = jax.nn.silu(normed_a).astype(jnp.bfloat16)
    mixer_out = blocked_product(activated, out_proj)
    features = tokens_b.astype(jnp.float32)
    normed_b = (features * lax.rsqrt(lax.optimization_barrier(jnp.mean(features * features, axis=1, keepdims=True)) + EPSILON) * norm_gain).astype(jnp.bfloat16)
    block_count = TOKENS_B // ROWS_DEV
    chosen, places = jax.vmap(partial(slot_table, expert_count=EXPERTS))(routes.reshape(block_count, ROWS_DEV * TOP_K))
    row_ids = jnp.arange(block_count, dtype=jnp.int32)[:, None] * ROWS_DEV + jnp.arange(ROWS_DEV * TOP_K, dtype=jnp.int32)[None, :] // TOP_K
    block_grid = jnp.broadcast_to(jnp.arange(block_count, dtype=jnp.int32)[:, None], row_ids.shape)
    slot_rows = jnp.zeros((EXPERTS, block_count, CAP), jnp.int32).at[chosen, block_grid, places].set(row_ids)
    slot_weights = jnp.zeros((EXPERTS, block_count, CAP), jnp.float32).at[chosen, block_grid, places].set(route_weights.reshape(block_count, ROWS_DEV * TOP_K))

    def per_expert(accumulated, inputs):
        weight_gate, weight_up, weight_down, rows_expert, weights_expert = inputs
        picked_ids = rows_expert.reshape(-1)
        outputs = gated_ffn(normed_b[picked_ids], weight_gate, weight_up, weight_down)
        accumulated = accumulated.at[picked_ids].add(outputs.astype(jnp.float32) * weights_expert.reshape(-1)[:, None])
        return (accumulated, None)
    routed, _ = lax.scan(per_expert, jnp.zeros((TOKENS_B, D), jnp.float32), (expert_gate, expert_up, expert_down, slot_rows, slot_weights))
    shared_rows = gated_ffn(normed_b, shared_gate, shared_up, shared_down)
    experts_out = (shared_rows.astype(jnp.float32) + routed).astype(jnp.bfloat16)
    return (mixer_out, experts_out)
```

```python
import jax
import jax.numpy as jnp
from jax import lax
from jax.sharding import PartitionSpec as P

EPSILON = 1e-06
COLUMN_CHUNKS = 2


def shifted(x, axis, by):
    devices = lax.axis_size(axis)
    pairs = [(i, i + by) for i in range(devices) if 0 <= i + by < devices]
    return lax.ppermute(x, axis, pairs)


def swapped(x, axis, bit):
    devices = lax.axis_size(axis)
    return lax.ppermute(x, axis, [(i, i ^ bit) for i in range(devices)])


def stages(axis):
    bits, bit = [], 1
    while bit < lax.axis_size(axis):
        bits.append(bit)
        bit *= 2
    return bits


def gathered(x, axis):
    pieces = [x]
    for bit in reversed(stages(axis)):
        pieces = pieces + [swapped(piece, axis, bit) for piece in pieces]
    return pieces


def scattered_product(lhs, weight, axis):
    count = lax.axis_size(axis)
    me = lax.axis_index(axis)
    bits = stages(axis)
    rows = lhs.shape[0] // count
    width = weight.shape[1]
    near = bits[0]
    core = me % 2
    blocks = lhs.reshape(count // 2, 2, rows, lhs.shape[1])
    sent = lax.dynamic_index_in_dim(blocks, 1 - core, 1, keepdims=False).reshape(-1, lhs.shape[1])
    kept = lax.dynamic_index_in_dim(blocks, core, 1, keepdims=False).reshape(-1, lhs.shape[1])
    sent = jnp.dot(sent, weight, preferred_element_type=jnp.float32).astype(jnp.bfloat16)
    arrived = swapped(sent, axis, near)
    kept = jnp.dot(kept, weight, preferred_element_type=jnp.float32).astype(jnp.bfloat16)
    total = (kept, arrived)
    left = count // 2
    for bit in bits[1:]:
        low = (me // bit) % 2
        halves = [part.reshape(left // 2, 2, rows, width) for part in total]
        give = [lax.dynamic_index_in_dim(h, 1 - low, 1, keepdims=False) for h in halves]
        keep = [lax.dynamic_index_in_dim(h, low, 1, keepdims=False) for h in halves]
        give = sum(g.astype(jnp.float32) for g in give).astype(jnp.bfloat16)
        total = tuple(keep) + (swapped(give, axis, bit),)
        left = left // 2
    return sum(part.reshape(rows, width).astype(jnp.float32) for part in total)


def rms_normed(features, gain):
    features = features.astype(jnp.float32)
    return (
        features
        * lax.rsqrt(jnp.mean(features * features, axis=1, keepdims=True) + EPSILON)
        * gain
    ).astype(jnp.bfloat16)


def gated_hidden(rows_in, weight_gate, weight_up):
    return (
        jax.nn.silu(jnp.dot(rows_in, weight_gate, preferred_element_type=jnp.float32))
        * jnp.dot(rows_in, weight_up, preferred_element_type=jnp.float32)
    ).astype(jnp.bfloat16)


def per_device(
    value_in,
    gate_in,
    conv_taps,
    conv_bias,
    ln_gain,
    ln_bias,
    out_proj,
    tokens_b,
    norm_gain,
    routes,
    route_weights,
    expert_gate,
    expert_up,
    expert_down,
    shared_gate,
    shared_up,
    shared_down,
):
    tp_count = lax.axis_size("tp")
    ep_count = lax.axis_size("ep")
    model_width = tokens_b.shape[1]
    rows_own, top_count = routes.shape
    capacity = max(2, 3 * rows_own * top_count // (2 * ep_count))

    gates = gathered(expert_gate[0], "tp")
    ups = gathered(expert_up[0], "tp")
    chunk = model_width // COLUMN_CHUNKS
    downs = [
        gathered(expert_down[0][:, c * chunk : (c + 1) * chunk], "tp")
        for c in range(COLUMN_CHUNKS)
    ]

    own = lax.dynamic_slice_in_dim(tokens_b, lax.axis_index("tp") * rows_own, rows_own, 0)
    own_rows = rms_normed(own, norm_gain)
    by_choice = routes.T
    expert_ids = jnp.arange(ep_count, dtype=jnp.int32)
    names = by_choice[:, None, :] == expert_ids[None, :, None]
    named = jnp.any(names, axis=0)
    row_ids = jnp.arange(rows_own, dtype=jnp.int32)
    before_row = (row_ids[:, None] < row_ids[None, :]).astype(jnp.bfloat16)
    earlier = jnp.dot(
        named.astype(jnp.bfloat16), before_row, preferred_element_type=jnp.float32
    ).astype(jnp.int32)
    slots = jnp.arange(capacity, dtype=jnp.int32)
    placed = earlier[:, None, :] == slots[None, :, None]
    pick = (placed & named[:, None, :]).astype(jnp.bfloat16).reshape(-1, rows_own)
    outbox = jnp.dot(pick, own_rows, preferred_element_type=jnp.float32).astype(jnp.bfloat16)
    arrived = lax.all_to_all(
        outbox.reshape(ep_count, capacity, model_width), "ep", split_axis=0, concat_axis=0, tiled=True
    ).reshape(ep_count * capacity, model_width)

    gated = (value_in.astype(jnp.float32) * jax.nn.sigmoid(gate_in.astype(jnp.float32))).astype(
        jnp.bfloat16
    )
    rim_rows = conv_taps.shape[0] - 1
    length = gated.shape[0]
    before = shifted(gated[length - rim_rows :], "ep", 1)
    padded = jnp.concatenate([before, gated], axis=0).astype(jnp.float32)
    filtered = jnp.zeros(gated.shape, jnp.float32) + conv_bias[None, :]
    for tap_index in range(rim_rows + 1):
        filtered = filtered + conv_taps[tap_index][None, :] * padded[tap_index : tap_index + length]
    row_sum, squares = lax.psum(
        (jnp.sum(filtered, axis=1), jnp.sum(filtered * filtered, axis=1)), "tp"
    )
    channel_count = filtered.shape[1] * tp_count
    average = row_sum / channel_count
    variance = squares / channel_count - average * average
    normed_a = (filtered - average[:, None]) * lax.rsqrt(
        variance[:, None] + EPSILON
    ) * ln_gain + ln_bias
    activated = jax.nn.silu(normed_a).astype(jnp.bfloat16)
    mixer_rows = scattered_product(activated, out_proj, "tp").astype(jnp.bfloat16)

    normed_b = rms_normed(tokens_b, norm_gain)
    hidden_shared = gated_hidden(normed_b, shared_gate, shared_up)
    shared_rows = scattered_product(hidden_shared, shared_down, "tp").astype(jnp.bfloat16)

    hidden = [gated_hidden(arrived, g, u) for g, u in zip(gates, ups)]
    parts = []
    for pieces in downs:
        product = sum(
            jnp.dot(h, piece, preferred_element_type=jnp.float32)
            for h, piece in zip(hidden, pieces)
        ).astype(jnp.bfloat16)
        parts.append(
            lax.all_to_all(
                product.reshape(ep_count, capacity, chunk),
                "ep",
                split_axis=0,
                concat_axis=0,
                tiled=True,
            ).reshape(ep_count * capacity, chunk)
        )
    outs = []
    for c, returned in enumerate(parts):
        total = shared_rows[:, c * chunk : (c + 1) * chunk].astype(jnp.float32)
        for k in range(top_count):
            choice = (placed & names[k][:, None, :]).astype(jnp.bfloat16).reshape(-1, rows_own)
            picked = lax.dot_general(
                choice, returned, (((0,), (0,)), ((), ())), preferred_element_type=jnp.float32
            )
            total = total + picked * route_weights[:, k][:, None]
        outs.append(total.astype(jnp.bfloat16))
    return (mixer_rows, jnp.concatenate(outs, axis=1))


def solution(mesh):
    return jax.shard_map(
        per_device,
        mesh=mesh,
        in_specs=(
            P("ep", "tp"),
            P("ep", "tp"),
            P(None, "tp"),
            P("tp"),
            P("tp"),
            P("tp"),
            P("tp", None),
            P("ep", None),
            P(),
            P(("ep", "tp"), None),
            P(("ep", "tp"), None),
            P("ep", None, "tp"),
            P("ep", None, "tp"),
            P("ep", "tp", None),
            P(None, "tp"),
            P(None, "tp"),
            P("tp", None),
        ),
        out_specs=(P(("ep", "tp"), None), P(("ep", "tp"), None)),
        check_vma=False,
    )
```

```python
import jax
import jax.numpy as jnp
from jax import lax
from jax.sharding import PartitionSpec as P

EPSILON = 1e-06
COLUMN_CHUNKS = 2


def shifted(x, axis, by):
    devices = lax.axis_size(axis)
    pairs = [(i, i + by) for i in range(devices) if 0 <= i + by < devices]
    return lax.ppermute(x, axis, pairs)


def swapped(x, axis, bit):
    devices = lax.axis_size(axis)
    return lax.ppermute(x, axis, [(i, i ^ bit) for i in range(devices)])


def stages(axis):
    bits, bit = [], 1
    while bit < lax.axis_size(axis):
        bits.append(bit)
        bit *= 2
    return bits


def gathered(x, axis):
    pieces = [x]
    for bit in reversed(stages(axis)):
        pieces = pieces + [swapped(piece, axis, bit) for piece in pieces]
    return pieces


def scattered_product(lhs, weight, axis):
    count = lax.axis_size(axis)
    me = lax.axis_index(axis)
    bits = stages(axis)
    rows = lhs.shape[0] // count
    width = weight.shape[1]
    near = bits[0]
    core = me % 2
    blocks = lhs.reshape(count // 2, 2, rows, lhs.shape[1])
    sent = lax.dynamic_index_in_dim(blocks, 1 - core, 1, keepdims=False).reshape(-1, lhs.shape[1])
    kept = lax.dynamic_index_in_dim(blocks, core, 1, keepdims=False).reshape(-1, lhs.shape[1])
    sent = jnp.dot(sent, weight, preferred_element_type=jnp.float32).astype(jnp.bfloat16)
    arrived = swapped(sent, axis, near)
    kept = jnp.dot(kept, weight, preferred_element_type=jnp.float32).astype(jnp.bfloat16)
    total = (kept, arrived)
    left = count // 2
    for bit in bits[1:]:
        low = (me // bit) % 2
        halves = [part.reshape(left // 2, 2, rows, width) for part in total]
        give = [lax.dynamic_index_in_dim(h, 1 - low, 1, keepdims=False) for h in halves]
        keep = [lax.dynamic_index_in_dim(h, low, 1, keepdims=False) for h in halves]
        give = sum(g.astype(jnp.float32) for g in give).astype(jnp.bfloat16)
        total = tuple(keep) + (swapped(give, axis, bit),)
        left = left // 2
    return sum(part.reshape(rows, width).astype(jnp.float32) for part in total)


def rms_normed(features, gain):
    features = features.astype(jnp.float32)
    return (
        features
        * lax.rsqrt(jnp.mean(features * features, axis=1, keepdims=True) + EPSILON)
        * gain
    ).astype(jnp.bfloat16)


def gated_hidden(rows_in, weight_gate, weight_up):
    return (
        jax.nn.silu(jnp.dot(rows_in, weight_gate, preferred_element_type=jnp.float32))
        * jnp.dot(rows_in, weight_up, preferred_element_type=jnp.float32)
    ).astype(jnp.bfloat16)


def per_device(
    value_in,
    gate_in,
    conv_taps,
    conv_bias,
    ln_gain,
    ln_bias,
    out_proj,
    tokens_b,
    norm_gain,
    routes,
    route_weights,
    expert_gate,
    expert_up,
    expert_down,
    shared_gate,
    shared_up,
    shared_down,
):
    tp_count = lax.axis_size("tp")
    ep_count = lax.axis_size("ep")
    model_width = tokens_b.shape[1]
    rows_own, top_count = routes.shape
    capacity = max(2, 3 * rows_own * top_count // (2 * ep_count))

    gates = gathered(expert_gate[0], "tp")
    ups = gathered(expert_up[0], "tp")
    chunk = model_width // COLUMN_CHUNKS

    own = lax.dynamic_slice_in_dim(tokens_b, lax.axis_index("tp") * rows_own, rows_own, 0)
    own_rows = rms_normed(own, norm_gain)
    by_choice = routes.T
    expert_ids = jnp.arange(ep_count, dtype=jnp.int32)
    names = by_choice[:, None, :] == expert_ids[None, :, None]
    named = jnp.any(names, axis=0)
    row_ids = jnp.arange(rows_own, dtype=jnp.int32)
    before_row = (row_ids[:, None] < row_ids[None, :]).astype(jnp.bfloat16)
    earlier = jnp.dot(
        named.astype(jnp.bfloat16), before_row, preferred_element_type=jnp.float32
    ).astype(jnp.int32)
    slots = jnp.arange(capacity, dtype=jnp.int32)
    placed = earlier[:, None, :] == slots[None, :, None]
    pick = (placed & named[:, None, :]).astype(jnp.bfloat16).reshape(-1, rows_own)
    outbox = jnp.dot(pick, own_rows, preferred_element_type=jnp.float32).astype(jnp.bfloat16)
    arrived = lax.all_to_all(
        outbox.reshape(ep_count, capacity, model_width), "ep", split_axis=0, concat_axis=0, tiled=True
    ).reshape(ep_count * capacity, model_width)

    gated = (value_in.astype(jnp.float32) * jax.nn.sigmoid(gate_in.astype(jnp.float32))).astype(
        jnp.bfloat16
    )
    rim_rows = conv_taps.shape[0] - 1
    length = gated.shape[0]
    before = shifted(gated[length - rim_rows :], "ep", 1)
    padded = jnp.concatenate([before, gated], axis=0).astype(jnp.float32)
    filtered = jnp.zeros(gated.shape, jnp.float32) + conv_bias[None, :]
    for tap_index in range(rim_rows + 1):
        filtered = filtered + conv_taps[tap_index][None, :] * padded[tap_index : tap_index + length]
    normed_b = rms_normed(tokens_b, norm_gain)
    hidden_shared = gated_hidden(normed_b, shared_gate, shared_up)
    shared_rows = scattered_product(hidden_shared, shared_down, "tp").astype(jnp.bfloat16)

    hidden = [gated_hidden(arrived, g, u) for g, u in zip(gates, ups)]
    parts, products = [], []
    for c in range(COLUMN_CHUNKS):
        local = expert_down[0][:, c * chunk : (c + 1) * chunk]
        if products:
            local, _ = lax.optimization_barrier((local, products[-1]))
        pieces = gathered(local, "tp")
        product = sum(
            jnp.dot(h, piece, preferred_element_type=jnp.float32)
            for h, piece in zip(hidden, pieces)
        ).astype(jnp.bfloat16)
        products.append(product)
        parts.append(
            lax.all_to_all(
                product.reshape(ep_count, capacity, chunk),
                "ep",
                split_axis=0,
                concat_axis=0,
                tiled=True,
            ).reshape(ep_count * capacity, chunk)
        )
    row_sum, squares, _ = lax.optimization_barrier(
        (jnp.sum(filtered, axis=1), jnp.sum(filtered * filtered, axis=1), products[0])
    )
    row_sum, squares = lax.psum((row_sum, squares), "tp")
    channel_count = filtered.shape[1] * tp_count
    average = row_sum / channel_count
    variance = squares / channel_count - average * average
    normed_a = (filtered - average[:, None]) * lax.rsqrt(
        variance[:, None] + EPSILON
    ) * ln_gain + ln_bias
    activated = jax.nn.silu(normed_a).astype(jnp.bfloat16)
    mixer_rows = scattered_product(activated, out_proj, "tp").astype(jnp.bfloat16)

    outs = []
    for c, returned in enumerate(parts):
        total = shared_rows[:, c * chunk : (c + 1) * chunk].astype(jnp.float32)
        for k in range(top_count):
            choice = (placed & names[k][:, None, :]).astype(jnp.bfloat16).reshape(-1, rows_own)
            picked = lax.dot_general(
                choice, returned, (((0,), (0,)), ((), ())), preferred_element_type=jnp.float32
            )
            total = total + picked * route_weights[:, k][:, None]
        outs.append(total.astype(jnp.bfloat16))
    return (mixer_rows, jnp.concatenate(outs, axis=1))


def solution(mesh):
    return jax.shard_map(
        per_device,
        mesh=mesh,
        in_specs=(
            P("ep", "tp"),
            P("ep", "tp"),
            P(None, "tp"),
            P("tp"),
            P("tp"),
            P("tp"),
            P("tp", None),
            P("ep", None),
            P(),
            P(("ep", "tp"), None),
            P(("ep", "tp"), None),
            P("ep", None, "tp"),
            P("ep", None, "tp"),
            P("ep", "tp", None),
            P(None, "tp"),
            P(None, "tp"),
            P("tp", None),
        ),
        out_specs=(P(("ep", "tp"), None), P(("ep", "tp"), None)),
        check_vma=False,
    )
```
